32 devices in a mesh: grp: 2 (over x), ep: 8 (over z, y), tp: 2 (over core).
Axes of the slice: x: 2, y: 2, z: 4, core: 2. Of those that a mesh axis runs over, the one named last changes fastest.
Arguments:
- tokens: bfloat16 [8192, 2048], P(('grp', 'ep', 'tp')), parts along dimension 0, may hold values from -6 to 6
- norm_gain: float32 [2048], replicated, may hold values from 0.1 to 1.9
- routes: int32 [8192, 3], P(('grp', 'ep', 'tp')), parts along dimension 0, may hold values from 0 to 7, all different within a row; in each aligned block of 256 rows (0 to 255, 256 to 511, ...) at most 144 rows name the same one
- gates: float32 [8192, 3], P(('grp', 'ep', 'tp')), parts along dimension 0, may hold values from 0.2 to 1.2
- expert_gate: bfloat16 [8, 2048, 512], P('ep', None, 'tp'), may hold values from -0.125 to 0.125
- expert_up: bfloat16 [8, 2048, 512], P('ep', None, 'tp'), may hold values from -0.125 to 0.125
- expert_down: bfloat16 [8, 512, 2048], P('ep', 'tp'), may hold values from -0.25 to 0.25
- shared_gate: bfloat16 [2048, 512], replicated, may hold values from -0.125 to 0.125
- shared_up: bfloat16 [2048, 512], replicated, may hold values from -0.125 to 0.125
- shared_down: bfloat16 [512, 2048], replicated, may hold values from -0.25 to 0.25
Outputs:
- mixed: bfloat16 [8192, 2048], P(('grp', 'ep', 'tp')), parts along dimension 0
The draws below stay inside these ranges and needn't reach their ends.
There are 2 independent parts, one for each index of `grp`. The reference program is written for one: setup_inputs(seed, part) draws one part's arguments, and reference() takes and returns one part's arrays. A program takes and returns all parts, laid end to end along the dimension named above; an argument that names none is the same for every part. Nothing has to cross between parts.
Inputs may be any that keep to these rules, and one draw needn't show every extreme that they name: `routes`: A row names 3 different experts. Among the rows of one device no expert is named by more than 144 rows, and in every draw some expert is named by exactly 144 rows of some device.
All inputs are finite; a program needn't handle non-finite values.
Results may differ from the reference program's by a relative error of at most 0.01.
Values may be sent and summed in bfloat16 or wider, within the bound.
No kernel may reach another device: no remote copies, remote signals or barrier semaphores. Data moves between devices by JAX's collectives and lax.ppermute only.
A program may use at most 128 MiB of HBM per device.

```python
import math
import jax
import jax.numpy as jnp
import numpy as np
from jax import lax

D = 2048
FE = 512
SH_FE = 512
TOP = 3
TOK_DEV = 256
EXPERTS = 8
CAP = 144
TOKENS = 4096
N_EP = 8
N_TP = 2


def level_of(stream_key, extent, pieces, low, top_value):
    factor_of = 1.0
    for dim, parts in pieces:
        draws = jax.random.uniform(jax.random.fold_in(jax.random.fold_in(stream_key, 6), dim), (parts,), jnp.float32, low / len(pieces), top_value / len(pieces))
        factor_of = factor_of * jnp.repeat(jnp.exp(draws), extent[dim] // parts).reshape((-1,) + (1,) * (len(extent) - 1 - dim))
    return factor_of


def routed_block(rng, own, number, rows, number_of, top, limit, skew):
    order = jax.random.permutation(rng, number_of)
    crowded, common = shares(number_of, rows * top, limit, skew, True), shares(number_of, rows * top, limit, skew, False)
    places = jnp.arange(number_of)

    def named(lengths, turn):
        used = int((lengths > 0).sum())
        fixed = max(1, used // 4)
        moved = fixed + (places - fixed + turn * (used - fixed)) % max(1, number_of - fixed)
        return jnp.zeros((number_of,), jnp.int32).at[order[jnp.where(places < fixed, places, moved)]].set(jnp.asarray(lengths, jnp.int32))

    lengths = jnp.where(number % 4 == 0, named(crowded, number // 4), named(common, number - number // 4 - 1))
    mixed = jax.random.permutation(jax.random.fold_in(own, 3), number_of)
    donor, taker = mixed[0:number_of // 2 * 2:2], mixed[1:number_of // 2 * 2:2]
    margin = jnp.minimum(lengths[donor] - 1, limit - lengths[taker]) // 2
    margin = jnp.where((donor == order[0]) | (taker == order[0]) | (lengths[taker] == 0), 0, jnp.maximum(margin, 0))
    moved = jax.random.randint(jax.random.fold_in(own, 4), (number_of // 2,), 0, 1 << 20) % (margin + 1)
    lengths = lengths.at[donor].add(-moved).at[taker].add(moved)
    labels = jnp.searchsorted(jnp.cumsum(lengths), jnp.arange(rows * top), side="right").astype(jnp.int32)
    listing = labels.reshape(top, rows).T
    listing = listing[jax.random.permutation(jax.random.fold_in(own, 1), rows)]
    turn = jax.random.randint(jax.random.fold_in(own, 2), (rows, 1), 0, top)
    return jnp.take_along_axis(listing, (jnp.arange(top)[None, :] + turn) % top, axis=1)


def shares(count, total, limit, skew, full):
    loads = [(1 << 20) // math.isqrt(rank ** skew) + 1 for rank in range(1, count + 1)]
    largest = limit if full else min(limit, max(-(-total // count), total * loads[0] // sum(loads)))
    least = 1 if total - largest >= count - 1 else 0
    given, spare = [largest] + [least] * (count - 1), total - largest - least * (count - 1)
    while spare > 0:
        free = [i for i in range(1, count) if given[i] < largest] or [i for i in range(1, count) if given[i] < limit]
        pool, left = sum([loads[i] for i in free]), spare
        for i in free:
            addition = min(limit - given[i], max(1, left * loads[i] // pool), spare)
            given[i] = given[i] + addition
            spare = spare - addition
    return np.array(given)


def scatter_about(stream_key, dims, deviation, limit, split=(), kind=jnp.bfloat16):
    array = jax.random.normal(stream_key, dims, jnp.float32) * deviation
    if len(split) > 0:
        array = level_of(stream_key, dims, split, -0.22, 0.18) * array
    return jnp.clip(array, min=-limit, max=limit).astype(kind)


def setup_inputs(seed: int = 0, part: int = 0) -> dict:
    splits = jax.random.split(jax.random.key(seed), 11)
    own_keys = jax.random.split(jax.random.fold_in(splits[10], part), 11)
    tokens = scatter_about(own_keys[0], (TOKENS, D), 1.0, 6.0, ((0, 16),))
    norm_gain = jnp.clip(1.0 + 0.18 * jax.random.normal(splits[1], (D,), jnp.float32), 0.1, 1.9)
    routes_keys = jax.random.split(jax.random.fold_in(own_keys[2], 1), TOKENS // TOK_DEV)
    routes_turns = jax.random.permutation(jax.random.fold_in(own_keys[2], 3), TOKENS // TOK_DEV)
    routes = jax.vmap(lambda own, number: routed_block(jax.random.fold_in(own_keys[2], 2), own, number, TOK_DEV, EXPERTS, TOP, CAP, 2))(routes_keys, routes_turns).reshape((TOKENS, TOP))
    gates = jnp.clip(0.2 + 1 * jax.random.uniform(own_keys[3], (TOKENS, TOP), jnp.float32) ** level_of(own_keys[3], (TOKENS, TOP), ((0, 16),), -0.2, 0.2), 0.2, 1.2)
    expert_gate = scatter_about(splits[4], (EXPERTS, D, FE), D ** -0.5, 0.125, ((0, 8), (2, 2)))
    expert_up = scatter_about(splits[5], (EXPERTS, D, FE), D ** -0.5, 0.125, ((0, 8), (2, 2)))
    expert_down = scatter_about(splits[6], (EXPERTS, FE, D), FE ** -0.5, 0.25, ((0, 8), (1, 2)))
    shared_gate = scatter_about(splits[7], (D, SH_FE), D ** -0.5, 0.125)
    shared_up = scatter_about(splits[8], (D, SH_FE), D ** -0.5, 0.125)
    shared_down = scatter_about(splits[9], (SH_FE, D), SH_FE ** -0.5, 0.25)
    return {"tokens": tokens, "norm_gain": norm_gain, "routes": routes, "gates": gates, "expert_gate": expert_gate, "expert_up": expert_up, "expert_down": expert_down, "shared_gate": shared_gate, "shared_up": shared_up, "shared_down": shared_down}


def reference(tokens, norm_gain, routes, gates, expert_gate, expert_up, expert_down, shared_gate, shared_up, shared_down):
    values = tokens.astype(jnp.float32)
    scaling = lax.rsqrt(lax.optimization_barrier(jnp.mean(values * values, axis=1, keepdims=True)) + 1e-06)
    normed = (values * scaling * norm_gain[None, :]).astype(jnp.bfloat16)
    shared_hidden = (jax.nn.silu(jnp.dot(normed, shared_gate, preferred_element_type=jnp.float32)) * jnp.dot(normed, shared_up, preferred_element_type=jnp.float32)).astype(jnp.bfloat16)
    shared_out = jnp.dot(shared_hidden, shared_down, preferred_element_type=jnp.float32)
    token_count = tokens.shape[0]
    top_count = routes.shape[1]
    flat_routes = routes.reshape(-1)
    bound = N_EP * N_TP * CAP
    padded = jnp.concatenate([normed, jnp.zeros((1, D), jnp.bfloat16)], axis=0)
    weights = jnp.concatenate([gates.reshape(-1), jnp.zeros((1,), jnp.float32)], axis=0)

    def one_expert(totals, expert_index):
        picks = jnp.nonzero(flat_routes == expert_index, size=bound, fill_value=token_count * top_count)[0].astype(jnp.int32)
        owners = (picks // top_count).astype(jnp.int32)
        chosen = padded[owners]
        hidden = (jax.nn.silu(jnp.dot(chosen, expert_gate[expert_index], preferred_element_type=jnp.float32)) * jnp.dot(chosen, expert_up[expert_index], preferred_element_type=jnp.float32)).astype(jnp.bfloat16)
        result = jnp.dot(hidden, expert_down[expert_index], preferred_element_type=jnp.float32).astype(jnp.bfloat16)
        weighted = result.astype(jnp.float32) * weights[picks][:, None]
        return (totals.at[owners].add(weighted), None)
    start_totals = jnp.zeros((token_count + 1, D), jnp.float32)
    totals, _ = lax.scan(one_expert, start_totals, jnp.arange(EXPERTS, dtype=jnp.int32))
    return (shared_out + totals[:token_count]).astype(jnp.bfloat16)
```

```python
import jax
import jax.numpy as jnp
from jax import lax
from jax.sharding import PartitionSpec as P

F32 = jnp.float32
BF16 = jnp.bfloat16


def dot(a, b):
    return jnp.dot(a, b, preferred_element_type=F32)


def slots_of(routes, first, count, capacity):
    rows = routes.shape[0]
    names = first + jnp.arange(count, dtype=jnp.int32)
    member = jnp.any(routes[:, :, None] == names[None, None, :], axis=1)
    before = jnp.arange(rows)[:, None] > jnp.arange(rows)[None, :]
    rank = dot(before.astype(BF16), member.astype(BF16)).astype(jnp.int32)
    rank = jnp.where(member, rank, -1).T
    onehot = rank[:, None, :] == jnp.arange(capacity, dtype=jnp.int32)[None, :, None]
    return onehot.reshape(count * capacity, rows)


def weights_of(onehot, routes, gates, first, count, capacity):
    names = first + jnp.arange(count, dtype=jnp.int32)
    chosen = routes[:, :, None] == names[None, None, :]
    scale = jnp.sum(jnp.where(chosen, gates[:, :, None], 0.0), axis=1).T
    high = lax.reduce_precision(scale, 8, 7)
    low = scale - high

    def spread(part):
        wide = jnp.repeat(part.astype(BF16), capacity, axis=0)
        return jnp.where(onehot, wide, jnp.zeros((), BF16))

    return spread(high), spread(low)


def combine(weights, back):
    high, low = weights
    dims = (((0,), (0,)), ((), ()))
    return lax.dot_general(high, back, dims, preferred_element_type=F32) + lax.dot_general(
        low, back, dims, preferred_element_type=F32
    )


def on_device(
    tokens,
    norm_gain,
    routes,
    gates,
    expert_gate,
    expert_up,
    expert_down,
    shared_gate,
    shared_up,
    shared_down,
):
    rows, width = tokens.shape
    top = routes.shape[1]
    local = expert_gate.shape[0]
    groups = lax.axis_size("ep")
    cores = lax.axis_size("tp")
    experts = local * groups
    capacity = 3 * rows * top // (2 * experts)
    half = groups // 2
    mine = experts // 2
    first = (lax.axis_index("ep") // half) * mine
    halves = [list(range(half)), list(range(half, groups))]
    across = [(i, (i + half) % groups) for i in range(groups)]

    values = tokens.astype(F32)
    scaling = lax.rsqrt(jnp.mean(values * values, axis=1, keepdims=True) + 1e-06)
    normed = (values * scaling * norm_gain[None, :]).astype(BF16)

    far_normed = lax.ppermute(normed, "ep", across)
    table = jnp.concatenate([routes.astype(F32), gates], axis=1)
    far_table = lax.ppermute(table, "ep", across)
    far_routes = far_table[:, :top].astype(jnp.int32)
    far_gates = far_table[:, top:]

    gate_parts, up_parts, down_parts = [expert_gate], [expert_up], [expert_down]
    for shift in range(1, cores):
        ring = [(i, (i + shift) % cores) for i in range(cores)]
        gate_parts.append(lax.ppermute(expert_gate, "tp", ring))
        up_parts.append(lax.ppermute(expert_up, "tp", ring))
        down_parts.append(lax.ppermute(expert_down, "tp", ring))

    def exchange(array):
        return lax.all_to_all(
            array, "ep", split_axis=0, concat_axis=0, tiled=True, axis_index_groups=halves
        )

    def send(onehot, source):
        picked = dot(onehot.astype(BF16), source).astype(BF16)
        return exchange(picked.reshape(half, local, capacity, width))

    def run(received):
        outs = []
        for e in range(local):
            x = received[:, e].reshape(half * capacity, width)
            total = None
            for g, u, d in zip(gate_parts, up_parts, down_parts):
                hidden = (jax.nn.silu(dot(x, g[e])) * dot(x, u[e])).astype(BF16)
                piece = dot(hidden, d[e])
                total = piece if total is None else total + piece
            outs.append(total.astype(BF16).reshape(half, capacity, width))
        return jnp.stack(outs, axis=1)

    near_slots = slots_of(routes, first, mine, capacity)
    near_in = send(near_slots, normed)

    shared_hidden = (
        jax.nn.silu(dot(normed, shared_gate)) * dot(normed, shared_up)
    ).astype(BF16)
    shared_out = dot(shared_hidden, shared_down)
    far_slots = slots_of(far_routes, first, mine, capacity).astype(BF16)
    far_normed, near_in, shared_out, far_slots, far_gates, gate_parts, up_parts, down_parts = (
        lax.optimization_barrier(
            (far_normed, near_in, shared_out, far_slots, far_gates, gate_parts, up_parts, down_parts)
        )
    )
    far_in = send(far_slots, far_normed)
    near_done = run(near_in)
    near_weights = weights_of(near_slots, routes, gates, first, mine, capacity)
    far_weights = weights_of(far_slots > 0, far_routes, far_gates, first, mine, capacity)
    far_in, near_done = lax.optimization_barrier((far_in, near_done))
    far_back = exchange(run(far_in))
    far_back, near_done = lax.optimization_barrier((far_back, near_done))
    near_back = exchange(near_done).reshape(mine * capacity, width)
    far_sum = combine(far_weights, far_back.reshape(mine * capacity, width))
    home = lax.ppermute(far_sum.astype(BF16), "ep", across)
    near_sum = combine(near_weights, near_back)
    return (shared_out + near_sum + home.astype(F32)).astype(BF16)


def solution(mesh):
    return jax.shard_map(
        on_device,
        mesh=mesh,
        in_specs=(
            P(("grp", "ep", "tp"), None),
            P(),
            P(("grp", "ep", "tp"), None),
            P(("grp", "ep", "tp"), None),
            P("ep", None, "tp"),
            P("ep", None, "tp"),
            P("ep", "tp", None),
            P(),
            P(),
            P(),
        ),
        out_specs=P(("grp", "ep", "tp"), None),
        check_vma=False,
    )
```

```python
import functools

import jax
import jax.numpy as jnp
from jax import lax
from jax.experimental import pallas as pl
from jax.experimental.pallas import tpu as pltpu
from jax.sharding import PartitionSpec as P

F32 = jnp.float32
BF16 = jnp.bfloat16


def dot(a, b):
    return jnp.dot(a, b, preferred_element_type=F32)


def slots_of(routes, first, count, capacity):
    rows = routes.shape[0]
    names = first + jnp.arange(count, dtype=jnp.int32)
    member = jnp.any(routes[:, :, None] == names[None, None, :], axis=1)
    before = jnp.arange(rows)[:, None] > jnp.arange(rows)[None, :]
    rank = dot(before.astype(BF16), member.astype(BF16)).astype(jnp.int32)
    rank = jnp.where(member, rank, -1).T
    onehot = rank[:, None, :] == jnp.arange(capacity, dtype=jnp.int32)[None, :, None]
    return onehot.reshape(count * capacity, rows)


def weights_of(onehot, routes, gates, first, count, capacity):
    names = first + jnp.arange(count, dtype=jnp.int32)
    chosen = routes[:, :, None] == names[None, None, :]
    scale = jnp.sum(jnp.where(chosen, gates[:, :, None], 0.0), axis=1).T
    wide = jnp.repeat(scale.astype(BF16), capacity, axis=0)
    return jnp.where(onehot, wide, jnp.zeros((), BF16))


def combine(weights, back):
    dims = (((0,), (0,)), ((), ()))
    return lax.dot_general(weights, back, dims, preferred_element_type=F32)


def expert_kernel(*refs, parts):
    x_ref, out_ref = refs[0], refs[-1]
    x = x_ref[...]
    hidden = []
    for p in range(parts):
        gate = dot(x, refs[1 + p][...])
        up = dot(x, refs[1 + parts + p][...])
        hidden.append((jax.nn.silu(gate) * up).astype(BF16))
    width = out_ref.shape[1]
    step = 256 if width % 256 == 0 else width
    for at in range(0, width, step):
        total = None
        for p in range(parts):
            piece = dot(hidden[p], refs[1 + 2 * parts + p][:, at : at + step])
            total = piece if total is None else total + piece
        out_ref[:, at : at + step] = total.astype(BF16)


def expert(x, gate_parts, up_parts, down_parts):
    parts = len(gate_parts)
    rows, width = x.shape
    units = gate_parts[0].shape[1]
    operands = [x, *gate_parts, *up_parts, *down_parts]
    return pl.pallas_call(
        functools.partial(expert_kernel, parts=parts),
        out_shape=jax.ShapeDtypeStruct((rows, width), BF16),
        in_specs=[pl.BlockSpec(memory_space=pltpu.VMEM)] * len(operands),
        out_specs=pl.BlockSpec(memory_space=pltpu.VMEM),
        cost_estimate=pl.CostEstimate(
            flops=6 * rows * width * units * parts,
            bytes_accessed=4 * rows * width + 6 * parts * width * units,
            transcendentals=rows * units * parts,
        ),
        compiler_params=pltpu.CompilerParams(vmem_limit_bytes=40 * 1024 * 1024),
        name="expert",
    )(*operands)


def on_device(
    tokens,
    norm_gain,
    routes,
    gates,
    expert_gate,
    expert_up,
    expert_down,
    shared_gate,
    shared_up,
    shared_down,
):
    rows, width = tokens.shape
    top = routes.shape[1]
    local = expert_gate.shape[0]
    groups = lax.axis_size("ep")
    cores = lax.axis_size("tp")
    experts = local * groups
    capacity = 3 * rows * top // (2 * experts)
    half = groups // 2
    mine = experts // 2
    first = (lax.axis_index("ep") // half) * mine
    halves = [list(range(half)), list(range(half, groups))]
    across = [(i, (i + half) % groups) for i in range(groups)]

    values = tokens.astype(F32)
    scaling = lax.rsqrt(jnp.mean(values * values, axis=1, keepdims=True) + 1e-06)
    normed = (values * scaling * norm_gain[None, :]).astype(BF16)

    far_normed = lax.ppermute(normed, "ep", across)
    table = jnp.concatenate([routes.astype(F32), gates], axis=1)
    far_table = lax.ppermute(table, "ep", across)
    far_routes = far_table[:, :top].astype(jnp.int32)
    far_gates = far_table[:, top:]

    gate_parts, up_parts, down_parts = [expert_gate], [expert_up], [expert_down]
    for shift in range(1, cores):
        ring = [(i, (i + shift) % cores) for i in range(cores)]
        gate_parts.append(lax.ppermute(expert_gate, "tp", ring))
        up_parts.append(lax.ppermute(expert_up, "tp", ring))
        down_parts.append(lax.ppermute(expert_down, "tp", ring))

    def exchange(array):
        return lax.all_to_all(
            array, "ep", split_axis=0, concat_axis=0, tiled=True, axis_index_groups=halves
        )

    def send(onehot, source):
        picked = dot(onehot.astype(BF16), source).astype(BF16)
        return exchange(picked.reshape(half, local, capacity, width))

    def run(received):
        outs = []
        for e in range(local):
            x = received[:, e].reshape(half * capacity, width)
            weights = ([part[e] for part in kind] for kind in (gate_parts, up_parts, down_parts))
            outs.append(expert(x, *weights).reshape(half, capacity, width))
        return jnp.stack(outs, axis=1)

    near_slots = slots_of(routes, first, mine, capacity)
    near_in = send(near_slots, normed)

    shared_hidden = (
        jax.nn.silu(dot(normed, shared_gate)) * dot(normed, shared_up)
    ).astype(BF16)
    shared_out = dot(shared_hidden, shared_down)
    far_slots = slots_of(far_routes, first, mine, capacity).astype(BF16)
    far_normed, near_in, shared_out, far_slots, far_gates, gate_parts, up_parts, down_parts = (
        lax.optimization_barrier(
            (far_normed, near_in, shared_out, far_slots, far_gates, gate_parts, up_parts, down_parts)
        )
    )
    far_in = send(far_slots, far_normed)
    near_done = run(near_in)
    near_weights = weights_of(near_slots, routes, gates, first, mine, capacity)
    far_weights = weights_of(far_slots > 0, far_routes, far_gates, first, mine, capacity)
    far_in, near_done = lax.optimization_barrier((far_in, near_done))
    far_back = exchange(run(far_in))
    far_back, near_done = lax.optimization_barrier((far_back, near_done))
    near_back = exchange(near_done).reshape(mine * capacity, width)
    far_sum = combine(far_weights, far_back.reshape(mine * capacity, width))
    home = lax.ppermute(far_sum.astype(BF16), "ep", across)
    near_back, home = lax.optimization_barrier((near_back, home))
    return (combine(near_weights, near_back) + (shared_out + home.astype(F32))).astype(BF16)


def solution(mesh):
    return jax.shard_map(
        on_device,
        mesh=mesh,
        in_specs=(
            P(("grp", "ep", "tp"), None),
            P(),
            P(("grp", "ep", "tp"), None),
            P(("grp", "ep", "tp"), None),
            P("ep", None, "tp"),
            P("ep", None, "tp"),
            P("ep", "tp", None),
            P(),
            P(),
            P(),
        ),
        out_specs=P(("grp", "ep", "tp"), None),
        check_vma=False,
    )
```

```python
import functools

import jax
import jax.numpy as jnp
from jax import lax
from jax.experimental import pallas as pl
from jax.experimental.pallas import tpu as pltpu
from jax.sharding import PartitionSpec as P

F32 = jnp.float32
BF16 = jnp.bfloat16


def dot(a, b):
    return jnp.dot(a, b, preferred_element_type=F32)


def slots_of(routes, first, count, capacity):
    rows = routes.shape[0]
    names = first + jnp.arange(count, dtype=jnp.int32)
    member = jnp.any(routes[:, :, None] == names[None, None, :], axis=1)
    before = jnp.arange(rows)[:, None] > jnp.arange(rows)[None, :]
    rank = dot(before.astype(BF16), member.astype(BF16)).astype(jnp.int32)
    rank = jnp.where(member, rank, -1).T
    onehot = rank[:, None, :] == jnp.arange(capacity, dtype=jnp.int32)[None, :, None]
    return onehot.reshape(count * capacity, rows)


def weights_of(onehot, routes, gates, first, count, capacity):
    names = first + jnp.arange(count, dtype=jnp.int32)
    chosen = routes[:, :, None] == names[None, None, :]
    scale = jnp.sum(jnp.where(chosen, gates[:, :, None], 0.0), axis=1).T
    wide = jnp.repeat(scale.astype(BF16), capacity, axis=0)
    return jnp.where(onehot, wide, jnp.zeros((), BF16))


def combine(weights, back):
    dims = (((0,), (0,)), ((), ()))
    return lax.dot_general(weights, back, dims, preferred_element_type=F32)


def expert_kernel(*refs, chunks, parts):
    xs, weights, outs = refs[:chunks], refs[chunks:-chunks], refs[-chunks:]
    span = xs[0].shape[1]

    def project(ref):
        total = None
        for c in range(chunks):
            piece = dot(xs[c][...], ref[c * span : (c + 1) * span, :])
            total = piece if total is None else total + piece
        return total

    hidden = []
    for p in range(parts):
        gate, up = project(weights[p]), project(weights[parts + p])
        hidden.append((jax.nn.silu(gate) * up).astype(BF16))
    step = 256 if span % 256 == 0 else span
    for c in range(chunks):
        for at in range(0, span, step):
            total = None
            for p in range(parts):
                low = c * span + at
                piece = dot(hidden[p], weights[2 * parts + p][:, low : low + step])
                total = piece if total is None else total + piece
            outs[c][:, at : at + step] = total.astype(BF16)


def expert(xs, gate_parts, up_parts, down_parts):
    parts, chunks = len(gate_parts), len(xs)
    rows, span = xs[0].shape
    width = span * chunks
    units = gate_parts[0].shape[1]
    operands = [*xs, *gate_parts, *up_parts, *down_parts]
    return pl.pallas_call(
        functools.partial(expert_kernel, chunks=chunks, parts=parts),
        out_shape=[jax.ShapeDtypeStruct((rows, span), BF16)] * chunks,
        in_specs=[pl.BlockSpec(memory_space=pltpu.VMEM)] * len(operands),
        out_specs=[pl.BlockSpec(memory_space=pltpu.VMEM)] * chunks,
        cost_estimate=pl.CostEstimate(
            flops=6 * rows * width * units * parts,
            bytes_accessed=4 * rows * width + 6 * parts * width * units,
            transcendentals=rows * units * parts,
        ),
        compiler_params=pltpu.CompilerParams(vmem_limit_bytes=40 * 1024 * 1024),
        name="expert",
    )(*operands)


def on_device(
    tokens,
    norm_gain,
    routes,
    gates,
    expert_gate,
    expert_up,
    expert_down,
    shared_gate,
    shared_up,
    shared_down,
):
    rows, width = tokens.shape
    top = routes.shape[1]
    local = expert_gate.shape[0]
    groups = lax.axis_size("ep")
    cores = lax.axis_size("tp")
    experts = local * groups
    capacity = 3 * rows * top // (2 * experts)
    half = groups // 2
    mine = experts // 2
    first = (lax.axis_index("ep") // half) * mine
    halves = [list(range(half)), list(range(half, groups))]
    across = [(i, (i + half) % groups) for i in range(groups)]

    values = tokens.astype(F32)
    scaling = lax.rsqrt(jnp.mean(values * values, axis=1, keepdims=True) + 1e-06)
    normed = (values * scaling * norm_gain[None, :]).astype(BF16)

    def columns(array):
        return [array[..., c * span : (c + 1) * span] for c in range(chunks)]

    chunks = 2 if width % 512 == 0 else 1
    span = width // chunks
    far_normed = []
    for piece in columns(normed):
        far_normed.append(lax.ppermute(piece, "ep", across))
    table = jnp.concatenate([routes.astype(F32), gates], axis=1)
    far_table = lax.ppermute(table, "ep", across)
    far_routes = far_table[:, :top].astype(jnp.int32)
    far_gates = far_table[:, top:]

    gate_parts, up_parts, down_parts = [expert_gate], [expert_up], [expert_down]
    for shift in range(1, cores):
        ring = [(i, (i + shift) % cores) for i in range(cores)]
        gate_parts.append(lax.ppermute(expert_gate, "tp", ring))
        up_parts.append(lax.ppermute(expert_up, "tp", ring))
        down_parts.append(lax.ppermute(expert_down, "tp", ring))

    def exchange(array):
        return lax.all_to_all(
            array, "ep", split_axis=0, concat_axis=0, tiled=True, axis_index_groups=halves
        )

    def send(onehot, source):
        picked = dot(onehot.astype(BF16), source).astype(BF16)
        return exchange(picked.reshape(half, local, capacity, source.shape[1]))

    def run(received):
        outs = []
        for e in range(local):
            xs = [piece[:, e].reshape(half * capacity, -1) for piece in received]
            weights = ([part[e] for part in kind] for kind in (gate_parts, up_parts, down_parts))
            outs.append([o.reshape(half, capacity, -1) for o in expert(xs, *weights)])
        return [jnp.stack([out[c] for out in outs], axis=1) for c in range(len(received))]

    def flat(back):
        return back.reshape(mine * capacity, back.shape[-1])

    near_slots = slots_of(routes, first, mine, capacity)
    near_in = send(near_slots, normed)

    shared_hidden = (
        jax.nn.silu(dot(normed, shared_gate)) * dot(normed, shared_up)
    ).astype(BF16)
    shared_out = dot(shared_hidden, shared_down)
    far_slots = slots_of(far_routes, first, mine, capacity).astype(BF16)
    far_normed[0], near_in, shared_out, far_slots, far_gates = lax.optimization_barrier(
        (far_normed[0], near_in, shared_out, far_slots, far_gates)
    )
    far_in = []
    for c in range(chunks):
        if c:
            far_normed[c], far_in[-1] = lax.optimization_barrier((far_normed[c], far_in[-1]))
        far_in.append(send(far_slots, far_normed[c]))
        if c == 0:
            far_in[0], gate_parts, up_parts, down_parts = lax.optimization_barrier(
                (far_in[0], gate_parts, up_parts, down_parts)
            )
    (near_done,) = run([near_in])
    near_weights = weights_of(near_slots, routes, gates, first, mine, capacity)
    far_weights = weights_of(far_slots > 0, far_routes, far_gates, first, mine, capacity)
    far_in, near_done, near_weights, far_weights = lax.optimization_barrier(
        (far_in, near_done, near_weights, far_weights)
    )
    far_done = run(far_in)
    homes = []
    for c in range(chunks):
        back = exchange(far_done[c])
        far_sum = combine(far_weights, flat(back)).astype(BF16)
        if c + 1 < chunks:
            far_sum, far_done[c + 1] = lax.optimization_barrier((far_sum, far_done[c + 1]))
        else:
            far_sum, near_done = lax.optimization_barrier((far_sum, near_done))
        homes.append(lax.ppermute(far_sum, "ep", across))
    near_back = exchange(near_done)
    near_back, homes = lax.optimization_barrier((near_back, homes))
    home = jnp.concatenate(homes, axis=1)
    return (combine(near_weights, flat(near_back)) + (shared_out + home.astype(F32))).astype(BF16)


def solution(mesh):
    return jax.shard_map(
        on_device,
        mesh=mesh,
        in_specs=(
            P(("grp", "ep", "tp"), None),
            P(),
            P(("grp", "ep", "tp"), None),
            P(("grp", "ep", "tp"), None),
            P("ep", None, "tp"),
            P("ep", None, "tp"),
            P("ep", "tp", None),
            P(),
            P(),
            P(),
        ),
        out_specs=P(("grp", "ep", "tp"), None),
        check_vma=False,
    )
```
